32 devices in a mesh: sp: 16 (over z, y, core), tp: 2 (over x).
Axes of the slice: x: 2, y: 2, z: 4, core: 2. Of those that a mesh axis runs over, the one named last changes fastest.
Arguments:
- target: bfloat16 [2048, 2048], P('sp'), may hold values from -0.375 to 0.375
- source: bfloat16 [4096, 2048], P(('sp', 'tp')), may hold values from -0.375 to 0.375
- target_gain: float32 [2048], replicated, may hold values from 0.3 to 12
- source_gain: float32 [2048], replicated, may hold values from 0.3 to 12
- w_query: bfloat16 [2048, 1024], P(None, 'tp'), may hold values from -0.125 to 0.125
- w_key: bfloat16 [2048, 256], replicated, may hold values from -0.125 to 0.125
- w_value: bfloat16 [2048, 256], replicated, may hold values from -0.125 to 0.125
- attended: bfloat16 [2048, 1024], P('sp', 'tp'), may hold values from -6 to 6
- d_attended: bfloat16 [2048, 1024], P('sp', 'tp'), may hold values from -24 to 24
Outputs:
- d_target: bfloat16 [2048, 2048], P('sp')
- d_source: float32 [4096, 2048], P(('sp', 'tp'))
- d_w_query: float32 [2048, 1024], P('sp', 'tp')
The draws below stay inside these ranges and needn't reach their ends.
All inputs are finite; a program needn't handle non-finite values.
Results may differ from the reference program's by a relative error of at most 0.02.
The reference program's roundings to bfloat16 on the way count: a program that leaves them out, or rounds other values in their place, can miss the bound.
Values may be sent and summed in bfloat16 or wider, within the bound.
A program may use at most 64 MiB of HBM per device.

```python
import jax
import jax.numpy as jnp
from jax import lax

D = 2048
HQ = 8
KVH = 2
HD = 128
TT = 2048
SS = 4096


def gain_law(key):
    return jax.random.uniform(key, (D,), jnp.float32, 0.3, 1.7)


def draw_target_gain(key, part):
    return gain_law(jax.random.fold_in(key, 11))


def draw_source_gain(key, part):
    return gain_law(jax.random.fold_in(key, 23))


def level_of(rng, extent, pieces, least, largest):
    factor_of = 1.0
    for position, parts in pieces:
        heights = jax.random.uniform(jax.random.fold_in(jax.random.fold_in(rng, 6), position), (parts,), jnp.float32, least / len(pieces), largest / len(pieces))
        factor_of = factor_of * jnp.repeat(jnp.exp(heights), extent[position] // parts).reshape((-1,) + (1,) * (len(extent) - 1 - position))
    return factor_of


def gaussian(key, dims, deviation, most, shards=(), held_as=jnp.bfloat16):
    loudness = level_of(key, dims, shards, -0.22, 0.18) if shards else 1.0
    array = jax.random.normal(key, dims, jnp.float32) * deviation * loudness
    return jnp.minimum(jnp.maximum(array, -most), most).astype(held_as)


def setup_inputs(seed: int = 0) -> dict:
    key_of = jax.random.split(jax.random.key(seed), 10)
    target = gaussian(key_of[0], (TT, D), 0.0625, 0.375, ((0, 16),))
    source = gaussian(key_of[1], (SS, D), 0.0625, 0.375, ((0, 32),))
    target_gain = draw_target_gain(jax.random.fold_in(key_of[9], 71), 0)
    source_gain = draw_source_gain(jax.random.fold_in(key_of[9], 71), 0)
    w_query = gaussian(key_of[4], (D, HQ * HD), D ** -0.5, 0.125, ((1, 2),))
    w_key = gaussian(key_of[5], (D, KVH * HD), D ** -0.5, 0.125)
    w_value = gaussian(key_of[6], (D, KVH * HD), D ** -0.5, 0.125)
    attended = gaussian(key_of[7], (TT, HQ * HD), 1.0, 6.0, ((0, 16), (1, 2)))
    d_attended = gaussian(key_of[8], (TT, HQ * HD), 4.0, 24.0, ((0, 16), (1, 2)))
    return {"target": target, "source": source, "target_gain": target_gain, "source_gain": source_gain, "w_query": w_query, "w_key": w_key, "w_value": w_value, "attended": attended, "d_attended": d_attended}


EPS = 1e-06

def norm_rows(matrix, gain_vector):
    widened = matrix.astype(jnp.float32)
    inverse = lax.rsqrt(lax.optimization_barrier(jnp.mean(widened * widened, axis=-1, keepdims=True)) + EPS)
    return widened * inverse * gain_vector

def norm_back(matrix, gain_vector, cotangent):
    _, pullback = jax.vjp(lambda values: norm_rows(values, gain_vector), matrix.astype(jnp.float32))
    return pullback(cotangent)[0]

def block_count(row_count, most_rows):
    number = 1
    while row_count % (number * 2) == 0 and row_count // number > most_rows:
        number = number * 2
    return number

def reference(target, source, target_gain, source_gain, w_query, w_key, w_value, attended, d_attended):
    scaling = HD ** (-0.5)
    group_size = HQ // KVH
    normed_target = norm_rows(target, target_gain).astype(jnp.bfloat16)
    normed_source = norm_rows(source, source_gain).astype(jnp.bfloat16)
    query = jnp.dot(normed_target, w_query, preferred_element_type=jnp.float32).astype(jnp.bfloat16)
    key = jnp.dot(normed_source, w_key, preferred_element_type=jnp.float32).astype(jnp.bfloat16)
    value = jnp.dot(normed_source, w_value, preferred_element_type=jnp.float32).astype(jnp.bfloat16)
    target_total = query.shape[0]
    source_total = key.shape[0]
    delta = lax.optimization_barrier(jnp.sum(d_attended.astype(jnp.float32).reshape(target_total, HQ, HD) * attended.astype(jnp.float32).reshape(target_total, HQ, HD), axis=-1)).astype(jnp.bfloat16)
    number = block_count(target_total, 512)
    block_rows = target_total // number

    def one_head(head_index):
        kv_index = head_index // group_size
        query_head = lax.dynamic_slice_in_dim(query, head_index * HD, HD, 1)
        key_head = lax.dynamic_slice_in_dim(key, kv_index * HD, HD, 1)
        value_head = lax.dynamic_slice_in_dim(value, kv_index * HD, HD, 1)
        grad_head = lax.dynamic_slice_in_dim(d_attended, head_index * HD, HD, 1)
        delta_head = lax.dynamic_slice_in_dim(delta, head_index, 1, 1)[:, 0]
        query_blocks = query_head.reshape(number, block_rows, HD)
        grad_blocks = grad_head.reshape(number, block_rows, HD)
        delta_blocks = delta_head.reshape(number, block_rows)

        def totals_of(queries):
            scores = jnp.dot(queries, key_head.T, preferred_element_type=jnp.float32) * scaling
            maxima = lax.optimization_barrier(jnp.max(scores, axis=-1))
            return maxima + jnp.log(lax.optimization_barrier(jnp.sum(jnp.exp(scores - maxima[:, None]), axis=-1)))
        log_total = lax.map(totals_of, query_blocks)

        def grad_step(carried, blocks):
            queries, cotangent, totals, delta_rows = blocks
            scores = jnp.dot(queries, key_head.T, preferred_element_type=jnp.float32) * scaling
            weights = jnp.exp(scores - totals[:, None])
            d_weights = jnp.dot(cotangent, value_head.T, preferred_element_type=jnp.float32)
            d_scores = (weights * (d_weights - delta_rows.astype(jnp.float32)[:, None])).astype(jnp.bfloat16)
            query_grad = jnp.dot(d_scores, key_head, preferred_element_type=jnp.float32) * scaling
            key_acc = carried[0] + jnp.dot(d_scores.T, queries, preferred_element_type=jnp.float32) * scaling
            value_acc = carried[1] + jnp.dot(weights.astype(jnp.bfloat16).T, cotangent, preferred_element_type=jnp.float32)
            return ((key_acc, value_acc), query_grad)
        start_state = (jnp.zeros((source_total, HD), jnp.float32), jnp.zeros((source_total, HD), jnp.float32))
        (key_acc, value_acc), query_grads = lax.scan(grad_step, start_state, (query_blocks, grad_blocks, log_total, delta_blocks))
        return (key_acc, value_acc, query_grads.reshape(target_total, HD))
    key_grads, value_grads, query_grads = lax.map(one_head, jnp.arange(HQ, dtype=jnp.int32))
    d_key = key_grads.reshape(KVH, group_size, source_total, HD).sum(axis=1)
    d_value = value_grads.reshape(KVH, group_size, source_total, HD).sum(axis=1)
    d_key_b = d_key.transpose(1, 0, 2).reshape(source_total, KVH * HD).astype(jnp.bfloat16)
    d_value_b = d_value.transpose(1, 0, 2).reshape(source_total, KVH * HD).astype(jnp.bfloat16)
    d_query_b = query_grads.transpose(1, 0, 2).reshape(target_total, HQ * HD).astype(jnp.bfloat16)
    d_w_query = jnp.dot(normed_target.T, d_query_b, preferred_element_type=jnp.float32)
    d_normed_target = jnp.dot(d_query_b, w_query.T, preferred_element_type=jnp.float32)
    d_target = norm_back(target, target_gain, d_normed_target).astype(jnp.bfloat16)
    d_normed_source = jnp.dot(d_key_b, w_key.T, preferred_element_type=jnp.float32) + jnp.dot(d_value_b, w_value.T, preferred_element_type=jnp.float32)
    d_source = norm_back(source, source_gain, d_normed_source)
    return (d_target, d_source, d_w_query)
```

```python
import functools

import jax
import jax.numpy as jnp
from jax import lax
from jax.experimental import pallas as pl
from jax.experimental.pallas import tpu as pltpu
from jax.sharding import PartitionSpec as P

KVH = 2
HD = 128
EPS = 1e-06
GROUP = 4
MESH = pl.DeviceIdType.MESH
F32 = jnp.float32
BF16 = jnp.bfloat16

NT_DIMS = (((1,), (1,)), ((), ()))


def dot_nn(a, b):
    return jnp.dot(a, b, preferred_element_type=F32)


def dot_nt(a, b):
    return lax.dot_general(a, b, NT_DIMS, preferred_element_type=F32)


def inverse_rms(x):
    return lax.rsqrt(jnp.mean(x * x, axis=-1, keepdims=True) + EPS)


def norm_back(x, gain, cotangent):
    inv = inverse_rms(x)
    gc = cotangent * gain
    inner = jnp.mean(x * gc, axis=-1, keepdims=True)
    return inv * gc - x * (inv * inv * inv * inner)


def kernel(
    sp_size,
    tp_size,
    target,
    source,
    tgain,
    sgain,
    wq,
    wk,
    wv,
    att,
    dout,
    dtarget,
    dsource,
    dwq,
    kvown,
    kvg,
    qg,
    og,
    delta,
    ntt,
    nttg,
    probs,
    cstat,
    stat,
    dks,
    dkg,
    dqacc,
    dqs,
    dqr,
    dqg,
    rets,
    ret,
    dnb,
    pacc,
    dws,
    dwg,
    tkv_s,
    tkv_r,
    lkv_s,
    lkv_r,
    in_s,
    in_r,
    st_s,
    st_r,
    dk_s,
    dk_r,
    dq_s,
    dq_r,
    ag_s,
    ag_r,
    rt_s,
    rt_r,
    dn_s,
    dn_r,
    dw_s,
    dw_r,
):
    outer = sp_size // GROUP
    rows = target.shape[0]
    width = wq.shape[1]
    heads = width // HD
    own_rows = source.shape[0]
    block = own_rows * tp_size
    group_rows = GROUP * rows
    scaling = HD ** (-0.5)
    sp = lax.axis_index("sp")
    t = lax.axis_index("tp")
    z = sp // GROUP
    g = sp % GROUP
    per_kv = tp_size // KVH

    def tp_peer(o):
        return lax.rem(t + o, tp_size)

    def g_peer(o):
        return lax.rem(g + o, GROUP)

    def z_peer(o):
        return lax.rem(z + o, outer)

    def to_tp(p):
        return {"sp": sp, "tp": p}

    def to_g(p):
        return {"sp": z * GROUP + p, "tp": t}

    def to_z(p):
        return {"sp": p * GROUP + g, "tp": t}

    def copy(src, dst, ssem, rsem, dev):
        return pltpu.make_async_remote_copy(
            src_ref=src, dst_ref=dst, send_sem=ssem, recv_sem=rsem, device_id=dev, device_id_type=MESH
        )

    barrier = pltpu.get_barrier_semaphore()
    for o in range(1, tp_size):
        pl.semaphore_signal(barrier, inc=1, device_id=to_tp(tp_peer(o)), device_id_type=MESH)
    for o in range(1, GROUP):
        pl.semaphore_signal(barrier, inc=1, device_id=to_g(g_peer(o)), device_id_type=MESH)
    for o in range(1, outer):
        pl.semaphore_signal(barrier, inc=1, device_id=to_z(z_peer(o)), device_id_type=MESH)
    pl.semaphore_wait(barrier, tp_size + GROUP + outer - 3)

    def group_copy(k, p, slot):
        src = (dout, qg.at[g], delta.at[g], ntt.at[:, p])[k]
        dst = (og, qg, delta, nttg)[k].at[slot]
        return copy(src, dst, in_s.at[k, p], in_r.at[k, slot], to_g(p))

    for o in range(1, GROUP):
        group_copy(0, g_peer(o), g).start()
    og[g] = dout[...]

    s32 = source[...].astype(F32)
    ns = (s32 * inverse_rms(s32) * sgain[...]).astype(BF16)
    keys = dot_nn(ns, wk[...]).astype(BF16)
    values = dot_nn(ns, wv[...]).astype(BF16)
    for c in range(KVH):
        kvown[c, :, 0:HD] = keys[:, c * HD : (c + 1) * HD]
        kvown[c, :, HD : 2 * HD] = values[:, c * HD : (c + 1) * HD]

    def tkv(p, slot):
        return copy(kvown.at[p // per_kv], kvg.at[z, slot], tkv_s.at[p], tkv_r.at[slot], to_tp(p))

    def lkv(p, zslot, tslot):
        return copy(
            kvg.at[z, tslot], kvg.at[zslot, tslot], lkv_s.at[p, tslot], lkv_r.at[zslot, tslot], to_z(p)
        )

    for o in range(1, tp_size):
        tkv(tp_peer(o), t).start()
    kvg[z, t] = kvown[t // per_kv]
    for o in range(1, outer):
        lkv(z_peer(o), z, t).start()

    t32 = target[...].astype(F32)
    nt32 = t32 * inverse_rms(t32) * tgain[...]
    qg[g] = dot_nn(nt32.astype(BF16), wq[...]).astype(BF16)
    prod = (dout[...].astype(F32) * att[...].astype(F32)).T
    drows = [jnp.sum(prod[h * HD : (h + 1) * HD], axis=0, keepdims=True) for h in range(heads)]
    drows.append(jnp.zeros((8 - heads, rows), F32))
    delta[g] = jnp.concatenate(drows, axis=0).astype(BF16).astype(F32)
    for k in (1, 2):
        for o in range(1, GROUP):
            group_copy(k, g_peer(o), g).start()
    for o in range(1, tp_size):
        p = tp_peer(o)
        tkv(t, p).wait_recv()
        for oz in range(1, outer):
            lkv(z_peer(oz), z, p).start()
    ntt[...] = nt32.T.astype(BF16).reshape(ntt.shape)
    for o in range(1, GROUP):
        group_copy(3, g_peer(o), g).start()
    nttg[g] = ntt[:, g]

    for k in (0, 1, 2):
        for o in range(1, GROUP):
            p = g_peer(o)
            group_copy(k, p, p).wait_recv()

    def columns(ref, h):
        return ref[:, :, h * HD : (h + 1) * HD].reshape(group_rows, HD)

    def first(o, _):
        zc = lax.rem(z + o, outer)

        @pl.when(o > 0)
        def _():
            for ts in range(tp_size):
                lkv(zc, zc, ts).wait_recv()

        kb = kvg[zc, :, :, 0:HD].reshape(block, HD)
        for h in range(heads):
            s = dot_nt(kb, columns(qg, h)) * scaling
            m = jnp.max(s, axis=0, keepdims=True)
            e = jnp.exp(s - m)
            probs[zc, h] = e
            cstat[zc, h : h + 1, :] = m
            cstat[zc, 8 + h : 9 + h, :] = jnp.sum(e, axis=0, keepdims=True)
        return 0

    lax.fori_loop(0, outer, first, 0)

    m_all = cstat[:, 0:heads, :]
    m_loc = jnp.max(m_all, axis=0)
    l_loc = jnp.sum(cstat[:, 8 : 8 + heads, :] * jnp.exp(m_all - m_loc[None]), axis=0)
    stat[g, 0:heads, :] = m_loc
    stat[g, 8 : 8 + heads, :] = l_loc
    if heads < 8:
        stat[g, heads:8, :] = jnp.zeros((8 - heads, group_rows), F32)
        stat[g, 8 + heads : 16, :] = jnp.zeros((8 - heads, group_rows), F32)

    def stat_copy(p, slot):
        return copy(stat.at[g], stat.at[slot], st_s.at[p], st_r.at[slot], to_g(p))

    for o in range(1, GROUP):
        stat_copy(g_peer(o), g).start()
    for o in range(1, GROUP):
        p = g_peer(o)
        stat_copy(p, p).wait_recv()
    m_g = jnp.max(stat[:, 0:heads, :], axis=0)
    l_g = jnp.sum(stat[:, 8 : 8 + heads, :] * jnp.exp(stat[:, 0:heads, :] - m_g[None]), axis=0)
    log_total = m_g + jnp.log(l_g)
    dqacc[...] = jnp.zeros_like(dqacc)

    def dk_copy(p, slot):
        return copy(dks.at[p], dkg.at[slot], dk_s.at[p], dk_r.at[slot], to_z(p))

    def second(o, _):
        zc = lax.rem(z + 1 + o, outer)
        kb = kvg[zc, :, :, 0:HD].reshape(block, HD)
        vb = kvg[zc, :, :, HD : 2 * HD].reshape(block, HD)
        kbt = kb.astype(F32).T.astype(BF16)
        dk = jnp.zeros((block, HD), F32)
        dv = jnp.zeros((block, HD), F32)
        for h in range(heads):
            qh = columns(qg, h)
            oh = columns(og, h)
            factor = jnp.exp(cstat[zc, h : h + 1, :] - log_total[h : h + 1, :])
            drow = jnp.concatenate([delta[i, h : h + 1, :] for i in range(GROUP)], axis=1)
            w = probs[zc, h] * factor
            ds = (w * (dot_nt(vb, oh) - drow)).astype(BF16)
            dk = dk + dot_nn(ds, qh)
            dv = dv + dot_nn(w.astype(BF16), oh)
            dqacc[h] += dot_nn(kbt, ds)
        dk = dk * scaling

        @pl.when(o < outer - 1)
        def _():
            dks[zc, :, 0:HD] = dk.astype(BF16)
            dks[zc, :, HD : 2 * HD] = dv.astype(BF16)
            dk_copy(zc, z).start()

        @pl.when(o == outer - 1)
        def _():
            pacc[:, 0:HD] = dk
            pacc[:, HD : 2 * HD] = dv

        return 0

    lax.fori_loop(0, outer, second, 0)

    def dq_copy(p, slot):
        return copy(dqs.at[p], dqr.at[slot], dq_s.at[p], dq_r.at[slot], to_g(p))

    dq_all = dqacc[...].reshape(width, group_rows) * scaling
    for i in range(GROUP):
        dqs[i] = dq_all[:, i * rows : (i + 1) * rows].astype(BF16)
    for o in range(1, GROUP):
        dq_copy(g_peer(o), g).start()

    for o in range(1, outer):
        p = z_peer(o)
        dk_copy(p, p).wait_recv()
    total = pacc[...]
    for o in range(1, outer):
        total = total + dkg[z_peer(o)].astype(F32)
    rets[...] = total.astype(BF16).reshape(rets.shape)

    def ret_copy(p, slot):
        return copy(rets.at[p], ret.at[slot], rt_s.at[p], rt_r.at[slot], to_tp(p))

    for o in range(1, tp_size):
        ret_copy(tp_peer(o), t).start()
    ret[t] = rets[t]

    dq_sum = dqs[g].astype(F32)
    for o in range(1, GROUP):
        p = g_peer(o)
        dq_copy(p, p).wait_recv()
        dq_sum = dq_sum + dqr[p].astype(F32)
    dq_own = dq_sum.T.astype(BF16)
    dqg[g] = dq_own

    def ag_copy(p, slot):
        return copy(dqg.at[g], dqg.at[slot], ag_s.at[p], ag_r.at[slot], to_g(p))

    def dn_copy(p, slot):
        return copy(dnb.at[t], dnb.at[slot], dn_s.at[p], dn_r.at[slot], to_tp(p))

    for o in range(1, GROUP):
        ag_copy(g_peer(o), g).start()
    dnb[t] = dot_nt(dq_own, wq[...]).astype(BF16)
    for o in range(1, tp_size):
        dn_copy(tp_peer(o), t).start()

    def dw_copy(p, slot):
        return copy(dws.at[p], dwg.at[slot], dw_s.at[p], dw_r.at[slot], to_z(p))

    depth = ntt.shape[2]
    term = dot_nn(nttg[g].reshape(outer * depth, rows), dq_own)
    for o in range(1, GROUP):
        p = g_peer(o)
        group_copy(3, p, p).wait_recv()
        ag_copy(p, p).wait_recv()
        term = term + dot_nn(nttg[p].reshape(outer * depth, rows), dqg[p])
    dws[...] = term.astype(BF16).reshape(dws.shape)
    for o in range(1, outer):
        dw_copy(z_peer(o), z).start()

    for o in range(1, tp_size):
        p = tp_peer(o)
        ret_copy(p, p).wait_recv()
    dns = jnp.zeros(source.shape, F32)
    for c in range(KVH):
        part = ret[c * per_kv].astype(F32)
        for k in range(1, per_kv):
            part = part + ret[c * per_kv + k].astype(F32)
        part = part.astype(BF16)
        dns = dns + dot_nt(part[:, 0:HD], wk[:, c * HD : (c + 1) * HD])
        dns = dns + dot_nt(part[:, HD : 2 * HD], wv[:, c * HD : (c + 1) * HD])
    dsource[...] = norm_back(source[...].astype(F32), sgain[...], dns)

    for o in range(1, tp_size):
        p = tp_peer(o)
        dn_copy(p, p).wait_recv()
    dn = dnb[0].astype(F32)
    for k in range(1, tp_size):
        dn = dn + dnb[k].astype(F32)
    dtarget[...] = norm_back(target[...].astype(F32), tgain[...], dn).astype(BF16)

    dw_total = dws[z].astype(F32)
    for o in range(1, outer):
        p = z_peer(o)
        dw_copy(p, p).wait_recv()
        dw_total = dw_total + dwg[p].astype(F32)
    dwq[...] = dw_total

    for o in range(1, tp_size):
        p = tp_peer(o)
        tkv(p, t).wait_send()
        ret_copy(p, t).wait_send()
        dn_copy(p, t).wait_send()
    for o in range(1, GROUP):
        p = g_peer(o)
        for k in range(4):
            group_copy(k, p, g).wait_send()
        stat_copy(p, g).wait_send()
        dq_copy(p, g).wait_send()
        ag_copy(p, g).wait_send()
    for o in range(1, outer):
        p = z_peer(o)
        for ts in range(tp_size):
            lkv(p, z, ts).wait_send()
        dk_copy(p, z).wait_send()
        dw_copy(p, z).wait_send()


def local(target, source, target_gain, source_gain, w_query, w_key, w_value, attended, d_attended):
    sp_size = lax.axis_size("sp")
    tp_size = lax.axis_size("tp")
    outer = sp_size // GROUP
    rows, d = target.shape
    own_rows = source.shape[0]
    block = own_rows * tp_size
    width = w_query.shape[1]
    heads = width // HD
    depth = d // sp_size
    group_rows = GROUP * rows
    vmem = pltpu.VMEM
    dma = pltpu.SemaphoreType.DMA
    scratch = [
        vmem((KVH, own_rows, 2 * HD), BF16),
        vmem((outer, tp_size, own_rows, 2 * HD), BF16),
        vmem((GROUP, rows, width), BF16),
        vmem((GROUP, rows, width), BF16),
        vmem((GROUP, 8, rows), F32),
        vmem((outer, GROUP, depth, rows), BF16),
        vmem((GROUP, outer, depth, rows), BF16),
        vmem((outer, heads, block, group_rows), F32),
        vmem((outer, 16, group_rows), F32),
        vmem((GROUP, 16, group_rows), F32),
        vmem((outer, block, 2 * HD), BF16),
        vmem((outer, block, 2 * HD), BF16),
        vmem((heads, HD, group_rows), F32),
        vmem((GROUP, width, rows), BF16),
        vmem((GROUP, width, rows), BF16),
        vmem((GROUP, rows, width), BF16),
        vmem((tp_size, own_rows, 2 * HD), BF16),
        vmem((tp_size, own_rows, 2 * HD), BF16),
        vmem((tp_size, rows, d), BF16),
        vmem((block, 2 * HD), F32),
        vmem((outer, depth, width), BF16),
        vmem((outer, depth, width), BF16),
    ]
    sems = [
        dma((tp_size,)),
        dma((tp_size,)),
        dma((outer, tp_size)),
        dma((outer, tp_size)),
        dma((4, GROUP)),
        dma((4, GROUP)),
    ]
    for n in (GROUP, outer, GROUP, GROUP, tp_size, tp_size, outer):
        sems += [dma((n,)), dma((n,))]
    spec = pl.BlockSpec(memory_space=pltpu.VMEM)
    return pl.pallas_call(
        functools.partial(kernel, sp_size, tp_size),
        out_shape=(
            jax.ShapeDtypeStruct((rows, d), BF16),
            jax.ShapeDtypeStruct((own_rows, d), F32),
            jax.ShapeDtypeStruct((depth, width), F32),
        ),
        in_specs=[spec] * 9,
        out_specs=(spec,) * 3,
        scratch_shapes=scratch + sems,
        compiler_params=pltpu.CompilerParams(
            collective_id=0, has_side_effects=True, vmem_limit_bytes=60000 * 1024
        ),
    )(
        target,
        source,
        target_gain.reshape(1, d),
        source_gain.reshape(1, d),
        w_query,
        w_key,
        w_value,
        attended,
        d_attended,
    )


def solution(mesh):
    return jax.shard_map(
        local,
        mesh=mesh,
        in_specs=(
            P("sp", None),
            P(("sp", "tp"), None),
            P(),
            P(),
            P(None, "tp"),
            P(),
            P(),
            P("sp", "tp"),
            P("sp", "tp"),
        ),
        out_specs=(P("sp", None), P(("sp", "tp"), None), P("sp", "tp")),
        check_vma=False,
    )
```

```python
import functools

import jax
import jax.numpy as jnp
from jax import lax
from jax.experimental import pallas as pl
from jax.experimental.pallas import tpu as pltpu
from jax.sharding import PartitionSpec as P

KVH = 2
HD = 128
EPS = 1e-06
GROUP = 4
MESH = pl.DeviceIdType.MESH
F32 = jnp.float32
BF16 = jnp.bfloat16

NT_DIMS = (((1,), (1,)), ((), ()))


def dot_nn(a, b):
    return jnp.dot(a, b, preferred_element_type=F32)


def dot_nt(a, b):
    return lax.dot_general(a, b, NT_DIMS, preferred_element_type=F32)


def inverse_rms(x):
    return lax.rsqrt(jnp.mean(x * x, axis=-1, keepdims=True) + EPS)


def norm_back(x, gain, cotangent):
    inv = inverse_rms(x)
    gc = cotangent * gain
    inner = jnp.mean(x * gc, axis=-1, keepdims=True)
    return inv * gc - x * (inv * inv * inv * inner)


def kernel(
    sp_size,
    tp_size,
    target_h,
    source_h,
    tgain_h,
    sgain_h,
    wq_h,
    wk_h,
    wv_h,
    att_h,
    dout_h,
    dtarget_h,
    dsource_h,
    dwq_h,
    target,
    source,
    tgain,
    sgain,
    wq,
    wk,
    wv,
    att,
    dtarget,
    dsource,
    dwq,
    ktg,
    kvown,
    kvg,
    qg,
    og,
    delta,
    ntt,
    nttg,
    probs,
    cstat,
    stat,
    dks,
    dkg,
    dqacc,
    dqs,
    dqr,
    dqg,
    rets,
    ret,
    dnb,
    dkacc,
    dws,
    dwg,
    tkv_s,
    tkv_r,
    lkv_s,
    lkv_r,
    in_s,
    in_r,
    nt_s,
    nt_r,
    st_s,
    st_r,
    dk_s,
    dk_r,
    dq_s,
    dq_r,
    ag_s,
    ag_r,
    rt_s,
    rt_r,
    dn_s,
    dn_r,
    dw_s,
    dw_r,
    ld_s,
    out_s,
):
    outer = sp_size // GROUP
    rows = target.shape[0]
    width = wq.shape[1]
    heads = width // HD
    own_rows = source.shape[0]
    block = own_rows * tp_size
    group_rows = GROUP * rows
    scaling = HD ** (-0.5)
    sp = lax.axis_index("sp")
    t = lax.axis_index("tp")
    z = sp // GROUP
    g = sp % GROUP
    per_kv = tp_size // KVH

    def tp_peer(o):
        return lax.rem(t + o, tp_size)

    def g_peer(o):
        return lax.rem(g + o, GROUP)

    def z_peer(o):
        return lax.rem(z + o, outer)

    def to_tp(p):
        return {"sp": sp, "tp": p}

    def to_g(p):
        return {"sp": z * GROUP + p, "tp": t}

    def to_z(p):
        return {"sp": p * GROUP + g, "tp": t}

    def copy(src, dst, ssem, rsem, dev):
        return pltpu.make_async_remote_copy(
            src_ref=src, dst_ref=dst, send_sem=ssem, recv_sem=rsem, device_id=dev, device_id_type=MESH
        )

    ga = g + 1 - 2 * lax.rem(g, 2)
    gb = lax.rem(g + 2, GROUP)
    gc = lax.rem(ga + 2, GROUP)
    parts = wq_parts(heads)
    part_heads = heads // parts
    part_width = width // parts

    loads = [
        pltpu.make_async_copy(src, dst, ld_s.at[n])
        for n, (src, dst) in enumerate(
            (
                (dout_h, og.at[g]),
                (source_h, source),
                (sgain_h, sgain),
                (wk_h, wk),
                (wv_h, wv),
                (target_h, target),
                (tgain_h, tgain),
                (wq_h, wq),
                (att_h, att),
            )
        )
    ]
    for load in loads:
        load.start()

    barrier = pltpu.get_barrier_semaphore()
    for o in range(1, tp_size):
        pl.semaphore_signal(barrier, inc=1, device_id=to_tp(tp_peer(o)), device_id_type=MESH)
    for o in range(1, GROUP):
        pl.semaphore_signal(barrier, inc=1, device_id=to_g(g_peer(o)), device_id_type=MESH)
    for o in range(1, outer):
        pl.semaphore_signal(barrier, inc=1, device_id=to_z(z_peer(o)), device_id_type=MESH)
    pl.semaphore_wait(barrier, tp_size + GROUP + outer - 3)

    def group_copy(k, way, slot):
        ref = (og, qg, delta)[k].at[slot]
        return copy(ref, ref, in_s.at[k, way], in_r.at[k, slot], to_g((ga, gb, ga)[way]))

    def send_own(k):
        group_copy(k, 1, g).start()
        group_copy(k, 0, g).start()

    def forward(k):
        group_copy(k, 1, gb).wait_recv()
        group_copy(k, 2, gb).start()

    def columns_copy(p, slot):
        return copy(ntt.at[:, p], nttg.at[slot], nt_s.at[p], nt_r.at[slot], to_g(p))

    loads[0].wait()
    send_own(0)
    for n in range(1, 5):
        loads[n].wait()

    s32 = source[...].astype(F32)
    ns = (s32 * inverse_rms(s32) * sgain[...]).astype(BF16)
    keys = dot_nn(ns, wk[...]).astype(BF16)
    values = dot_nn(ns, wv[...]).astype(BF16)
    for c in range(KVH):
        kvown[c, :, 0:HD] = keys[:, c * HD : (c + 1) * HD]
        kvown[c, :, HD : 2 * HD] = values[:, c * HD : (c + 1) * HD]

    def tkv(p, slot):
        return copy(kvown.at[p // per_kv], kvg.at[z, slot], tkv_s.at[p], tkv_r.at[slot], to_tp(p))

    def lkv(p, zslot, tslot):
        return copy(
            kvg.at[z, tslot], kvg.at[zslot, tslot], lkv_s.at[p, tslot], lkv_r.at[zslot, tslot], to_z(p)
        )

    for o in range(1, tp_size):
        tkv(tp_peer(o), t).start()
    kvg[z, t] = kvown[t // per_kv]
    for o in range(1, outer):
        lkv(z_peer(o), z, t).start()

    for n in range(5, 9):
        loads[n].wait()
    t32 = target[...].astype(F32)
    nt32 = t32 * inverse_rms(t32) * tgain[...]
    qg[g] = dot_nn(nt32.astype(BF16), wq[...]).astype(BF16)
    send_own(1)
    prod = (og[g].astype(F32) * att[...].astype(F32)).T
    drows = [jnp.sum(prod[h * HD : (h + 1) * HD], axis=0, keepdims=True) for h in range(heads)]
    drows.append(jnp.zeros((8 - heads, rows), F32))
    delta[g] = jnp.concatenate(drows, axis=0).astype(BF16).astype(F32)
    send_own(2)
    for o in range(1, tp_size):
        p = tp_peer(o)
        tkv(t, p).wait_recv()
        for oz in range(1, outer):
            lkv(z_peer(oz), z, p).start()
    forward(0)
    forward(1)
    forward(2)
    ntt[...] = nt32.T.astype(BF16).reshape(ntt.shape)
    for p in (gc, gb, ga):
        columns_copy(p, g).start()
    nttg[g] = ntt[:, g]
    for p in (ga, gc):
        group_copy(1, 0, p).wait_recv()

    def columns(ref, h):
        return ref[:, :, h * HD : (h + 1) * HD].reshape(group_rows, HD)

    def first(o, _):
        zc = lax.rem(z + o, outer)

        @pl.when(o > 0)
        def _():
            for ts in range(tp_size):
                lkv(zc, zc, ts).wait_recv()

        kb = kvg[zc, :, :, 0:HD].reshape(block, HD)
        ktg[zc] = kb.astype(F32).T.astype(BF16)
        for h in range(heads):
            s = dot_nt(kb, columns(qg, h)) * scaling
            m = jnp.max(s, axis=0, keepdims=True)
            e = jnp.exp(s - m)
            probs[zc, h] = e
            cstat[zc, h : h + 1, :] = m
            cstat[zc, 8 + h : 9 + h, :] = jnp.sum(e, axis=0, keepdims=True)
        return 0

    lax.fori_loop(0, outer, first, 0)

    m_all = cstat[:, 0:heads, :]
    m_loc = jnp.max(m_all, axis=0)
    l_loc = jnp.sum(cstat[:, 8 : 8 + heads, :] * jnp.exp(m_all - m_loc[None]), axis=0)
    stat[g, 0:heads, :] = m_loc
    stat[g, 8 : 8 + heads, :] = l_loc
    if heads < 8:
        stat[g, heads:8, :] = jnp.zeros((8 - heads, group_rows), F32)
        stat[g, 8 + heads : 16, :] = jnp.zeros((8 - heads, group_rows), F32)

    def stat_copy(p, slot):
        return copy(stat.at[g], stat.at[slot], st_s.at[p], st_r.at[slot], to_g(p))

    for o in range(1, GROUP):
        stat_copy(g_peer(o), g).start()
    for o in range(1, GROUP):
        p = g_peer(o)
        stat_copy(p, p).wait_recv()
    m_g = jnp.max(stat[:, 0:heads, :], axis=0)
    l_g = jnp.sum(stat[:, 8 : 8 + heads, :] * jnp.exp(stat[:, 0:heads, :] - m_g[None]), axis=0)
    log_total = m_g + jnp.log(l_g)
    dqacc[...] = jnp.zeros_like(dqacc)
    for k in (0, 2):
        for p in (ga, gc):
            group_copy(k, 0, p).wait_recv()

    def dk_copy(p, slot):
        return copy(dks.at[p], dkg.at[slot], dk_s.at[p], dk_r.at[slot], to_z(p))

    def dq_copy(k, p, slot):
        return copy(dqs.at[k, p], dqr.at[k, slot], dq_s.at[k, p], dq_r.at[k, slot], to_g(p))

    for k in range(parts):

        def second(o, _):
            zc = lax.rem(z + 1 + o, outer)
            vb = kvg[zc, :, :, HD : 2 * HD].reshape(block, HD)
            kbt = ktg[zc]
            dk = jnp.zeros((block, HD), F32)
            dv = jnp.zeros((block, HD), F32)
            for h in range(k * part_heads, (k + 1) * part_heads):
                qh = columns(qg, h)
                oh = columns(og, h)
                factor = jnp.exp(cstat[zc, h : h + 1, :] - log_total[h : h + 1, :])
                drow = jnp.concatenate([delta[i, h : h + 1, :] for i in range(GROUP)], axis=1)
                w = probs[zc, h] * factor
                ds = (w * (dot_nt(vb, oh) - drow)).astype(BF16)
                dk = dk + dot_nn(ds, qh)
                dv = dv + dot_nn(w.astype(BF16), oh)
                dqacc[h] += dot_nn(kbt, ds)
            dk = dk * scaling
            if k > 0:
                dk = dk + dkacc[zc, :, 0:HD]
                dv = dv + dkacc[zc, :, HD : 2 * HD]
            dkacc[zc, :, 0:HD] = dk
            dkacc[zc, :, HD : 2 * HD] = dv
            if k == parts - 1:

                @pl.when(o < outer - 1)
                def _():
                    dks[zc, :, 0:HD] = dk.astype(BF16)
                    dks[zc, :, HD : 2 * HD] = dv.astype(BF16)
                    dk_copy(zc, z).start()

            return 0

        lax.fori_loop(0, outer, second, 0)

        for i in range(GROUP):
            for h in range(part_heads):
                dqs[k, i, h * HD : (h + 1) * HD] = (
                    dqacc[k * part_heads + h, :, i * rows : (i + 1) * rows] * scaling
                ).astype(BF16)
        for p in (gc, gb, ga):
            dq_copy(k, p, g).start()

    def ag_copy(k, way, slot):
        ref = dqg.at[k, slot]
        return copy(ref, ref, ag_s.at[k, way], ag_r.at[k, slot], to_g((ga, gb, ga)[way]))

    dn_term = jnp.zeros((rows, wq.shape[0]), F32)
    for k in range(parts):
        dq_sum = dqs[k, g].astype(F32)
        for p in (ga, gb, gc):
            dq_copy(k, p, p).wait_recv()
            dq_sum = dq_sum + dqr[k, p].astype(F32)
        dqg[k, g] = dq_sum.T.astype(BF16)
        ag_copy(k, 1, g).start()
        ag_copy(k, 0, g).start()

    def dn_copy(p, slot):
        return copy(dnb.at[t], dnb.at[slot], dn_s.at[p], dn_r.at[slot], to_tp(p))

    for k in range(parts):
        dn_term = dn_term + dot_nt(dqg[k, g], wq[:, k * part_width : (k + 1) * part_width])
    dnb[t] = dn_term.astype(BF16)
    for o in range(1, tp_size):
        dn_copy(tp_peer(o), t).start()
    for k in range(parts):
        ag_copy(k, 1, gb).wait_recv()
        ag_copy(k, 2, gb).start()

    def dw_copy(k, p, slot):
        return copy(dws.at[k, p], dwg.at[k, slot], dw_s.at[k, p], dw_r.at[k, slot], to_z(p))

    depth = ntt.shape[2]

    def normed_columns(i):
        return nttg[i].reshape(outer * depth, rows)

    for p in (ga, gb, gc):
        columns_copy(p, p).wait_recv()
    for k in range(parts):
        term = dot_nn(normed_columns(g), dqg[k, g]) + dot_nn(normed_columns(gb), dqg[k, gb])
        for p in (ga, gc):
            ag_copy(k, 0, p).wait_recv()
            term = term + dot_nn(normed_columns(p), dqg[k, p])
        dws[k] = term.astype(BF16).reshape(dws.shape[1:])
        for o in range(1, outer):
            dw_copy(k, z_peer(o), z).start()

    for o in range(1, outer):
        p = z_peer(o)
        dk_copy(p, p).wait_recv()
    total = dkacc[z]
    for o in range(1, outer):
        total = total + dkg[z_peer(o)].astype(F32)
    rets[...] = total.astype(BF16).reshape(rets.shape)

    def ret_copy(p, slot):
        return copy(rets.at[p], ret.at[slot], rt_s.at[p], rt_r.at[slot], to_tp(p))

    for o in range(1, tp_size):
        ret_copy(tp_peer(o), t).start()
    ret[t] = rets[t]

    for o in range(1, tp_size):
        p = tp_peer(o)
        ret_copy(p, p).wait_recv()
    dns = jnp.zeros(source.shape, F32)
    for c in range(KVH):
        part = ret[c * per_kv].astype(F32)
        for k in range(1, per_kv):
            part = part + ret[c * per_kv + k].astype(F32)
        part = part.astype(BF16)
        dns = dns + dot_nt(part[:, 0:HD], wk[:, c * HD : (c + 1) * HD])
        dns = dns + dot_nt(part[:, HD : 2 * HD], wv[:, c * HD : (c + 1) * HD])
    dsource[...] = norm_back(source[...].astype(F32), sgain[...], dns)
    stores = [
        pltpu.make_async_copy(src, dst, out_s.at[n])
        for n, (src, dst) in enumerate(((dsource, dsource_h), (dtarget, dtarget_h), (dwq, dwq_h)))
    ]
    stores[0].start()

    for o in range(1, tp_size):
        p = tp_peer(o)
        dn_copy(p, p).wait_recv()
    dn = dnb[0].astype(F32)
    for k in range(1, tp_size):
        dn = dn + dnb[k].astype(F32)
    dtarget[...] = norm_back(target[...].astype(F32), tgain[...], dn).astype(BF16)

    stores[1].start()

    for k in range(parts):
        dw_total = dws[k, z].astype(F32)
        for o in range(1, outer):
            p = z_peer(o)
            dw_copy(k, p, p).wait_recv()
            dw_total = dw_total + dwg[k, p].astype(F32)
        dwq[:, k * part_width : (k + 1) * part_width] = dw_total
    stores[2].start()

    for o in range(1, tp_size):
        p = tp_peer(o)
        tkv(p, t).wait_send()
        ret_copy(p, t).wait_send()
        dn_copy(p, t).wait_send()
    for k in range(3):
        group_copy(k, 0, g).wait_send()
        group_copy(k, 1, g).wait_send()
        group_copy(k, 2, gb).wait_send()
    for p in (ga, gb, gc):
        columns_copy(p, g).wait_send()
        stat_copy(p, g).wait_send()
        for k in range(parts):
            dq_copy(k, p, g).wait_send()
    for k in range(parts):
        ag_copy(k, 0, g).wait_send()
        ag_copy(k, 1, g).wait_send()
        ag_copy(k, 2, gb).wait_send()
    for o in range(1, outer):
        p = z_peer(o)
        for ts in range(tp_size):
            lkv(p, z, ts).wait_send()
        dk_copy(p, z).wait_send()
        for k in range(parts):
            dw_copy(k, p, z).wait_send()
    for store in stores:
        store.wait()


def wq_parts(heads):
    return 2 if heads % 2 == 0 else 1


def local(target, source, target_gain, source_gain, w_query, w_key, w_value, attended, d_attended):
    sp_size = lax.axis_size("sp")
    tp_size = lax.axis_size("tp")
    outer = sp_size // GROUP
    rows, d = target.shape
    own_rows = source.shape[0]
    block = own_rows * tp_size
    width = w_query.shape[1]
    heads = width // HD
    depth = d // sp_size
    group_rows = GROUP * rows
    vmem = pltpu.VMEM
    dma = pltpu.SemaphoreType.DMA
    parts = wq_parts(heads)
    part_width = width // parts
    scratch = [
        vmem((rows, d), BF16),
        vmem((own_rows, d), BF16),
        vmem((1, d), F32),
        vmem((1, d), F32),
        vmem((d, width), BF16),
        vmem(w_key.shape, BF16),
        vmem(w_value.shape, BF16),
        vmem((rows, width), BF16),
        vmem((rows, d), BF16),
        vmem((own_rows, d), F32),
        vmem((depth, width), F32),
        vmem((outer, HD, block), BF16),
        vmem((KVH, own_rows, 2 * HD), BF16),
        vmem((outer, tp_size, own_rows, 2 * HD), BF16),
        vmem((GROUP, rows, width), BF16),
        vmem((GROUP, rows, width), BF16),
        vmem((GROUP, 8, rows), F32),
        vmem((outer, GROUP, depth, rows), BF16),
        vmem((GROUP, outer, depth, rows), BF16),
        vmem((outer, heads, block, group_rows), F32),
        vmem((outer, 16, group_rows), F32),
        vmem((GROUP, 16, group_rows), F32),
        vmem((outer, block, 2 * HD), BF16),
        vmem((outer, block, 2 * HD), BF16),
        vmem((heads, HD, group_rows), F32),
        vmem((parts, GROUP, part_width, rows), BF16),
        vmem((parts, GROUP, part_width, rows), BF16),
        vmem((parts, GROUP, rows, part_width), BF16),
        vmem((tp_size, own_rows, 2 * HD), BF16),
        vmem((tp_size, own_rows, 2 * HD), BF16),
        vmem((tp_size, rows, d), BF16),
        vmem((outer, block, 2 * HD), F32),
        vmem((parts, outer, depth, part_width), BF16),
        vmem((parts, outer, depth, part_width), BF16),
    ]
    sems = [
        dma((tp_size,)),
        dma((tp_size,)),
        dma((outer, tp_size)),
        dma((outer, tp_size)),
        dma((3, 3)),
        dma((3, GROUP)),
        dma((GROUP,)),
        dma((GROUP,)),
        dma((GROUP,)),
        dma((GROUP,)),
        dma((outer,)),
        dma((outer,)),
        dma((parts, GROUP)),
        dma((parts, GROUP)),
        dma((parts, 3)),
        dma((parts, GROUP)),
        dma((tp_size,)),
        dma((tp_size,)),
        dma((tp_size,)),
        dma((tp_size,)),
        dma((parts, outer)),
        dma((parts, outer)),
        dma((9,)),
        dma((3,)),
    ]
    spec = pl.BlockSpec(memory_space=pl.ANY)
    return pl.pallas_call(
        functools.partial(kernel, sp_size, tp_size),
        out_shape=(
            jax.ShapeDtypeStruct((rows, d), BF16),
            jax.ShapeDtypeStruct((own_rows, d), F32),
            jax.ShapeDtypeStruct((depth, width), F32),
        ),
        in_specs=[spec] * 9,
        out_specs=(spec,) * 3,
        scratch_shapes=scratch + sems,
        compiler_params=pltpu.CompilerParams(
            collective_id=0, has_side_effects=True, vmem_limit_bytes=60000 * 1024
        ),
    )(
        target,
        source,
        target_gain.reshape(1, d),
        source_gain.reshape(1, d),
        w_query,
        w_key,
        w_value,
        attended,
        d_attended,
    )


def solution(mesh):
    return jax.shard_map(
        local,
        mesh=mesh,
        in_specs=(
            P("sp", None),
            P(("sp", "tp"), None),
            P(),
            P(),
            P(None, "tp"),
            P(),
            P(),
            P("sp", "tp"),
            P("sp", "tp"),
        ),
        out_specs=(P("sp", None), P(("sp", "tp"), None), P("sp", "tp")),
        check_vma=False,
    )
```

```python
import functools

import jax
import jax.numpy as jnp
from jax import lax
from jax.experimental import pallas as pl
from jax.experimental.pallas import tpu as pltpu
from jax.sharding import PartitionSpec as P

KVH = 2
HD = 128
EPS = 1e-06
GROUP = 4
MESH = pl.DeviceIdType.MESH
F32 = jnp.float32
BF16 = jnp.bfloat16

NT_DIMS = (((1,), (1,)), ((), ()))


def dot_nn(a, b):
    return jnp.dot(a, b, preferred_element_type=F32)


def dot_nt(a, b):
    return lax.dot_general(a, b, NT_DIMS, preferred_element_type=F32)


def inverse_rms(x):
    return lax.rsqrt(jnp.mean(x * x, axis=-1, keepdims=True) + EPS)


def norm_back(x, gain, cotangent):
    inv = inverse_rms(x)
    gc = cotangent * gain
    inner = jnp.mean(x * gc, axis=-1, keepdims=True)
    return inv * gc - x * (inv * inv * inv * inner)


def kernel(
    sp_size,
    tp_size,
    target_h,
    source_h,
    tgain_h,
    sgain_h,
    wq_h,
    wk_h,
    wv_h,
    att_h,
    dout_h,
    dtarget_h,
    dsource_h,
    dwq_h,
    target,
    source,
    tgain,
    sgain,
    wq,
    wk,
    wv,
    att,
    dtarget,
    dsource,
    dwq,
    ktg,
    kvown,
    kvg,
    qg,
    og,
    delta,
    ntt,
    nttg,
    probs,
    prods,
    cstat,
    stat,
    dks,
    dkg,
    dqacc,
    dqs,
    dqr,
    dqg,
    rets,
    ret,
    dnb,
    dkacc,
    dws,
    dwg,
    tkv_s,
    tkv_r,
    lkv_s,
    lkv_r,
    in_s,
    in_r,
    nt_s,
    nt_r,
    st_s,
    st_r,
    dk_s,
    dk_r,
    dq_s,
    dq_r,
    ag_s,
    ag_r,
    rt_s,
    rt_r,
    dn_s,
    dn_r,
    dw_s,
    dw_r,
    ld_s,
    out_s,
):
    outer = sp_size // GROUP
    rows = target.shape[0]
    width = wq.shape[1]
    heads = width // HD
    own_rows = source.shape[0]
    block = own_rows * tp_size
    group_rows = GROUP * rows
    scaling = HD ** (-0.5)
    sp = lax.axis_index("sp")
    t = lax.axis_index("tp")
    z = sp // GROUP
    g = sp % GROUP
    per_kv = tp_size // KVH

    def tp_peer(o):
        return lax.rem(t + o, tp_size)

    def g_peer(o):
        return lax.rem(g + o, GROUP)

    def z_peer(o):
        return lax.rem(z + o, outer)

    def to_tp(p):
        return {"sp": sp, "tp": p}

    def to_g(p):
        return {"sp": z * GROUP + p, "tp": t}

    def to_z(p):
        return {"sp": p * GROUP + g, "tp": t}

    def copy(src, dst, ssem, rsem, dev):
        return pltpu.make_async_remote_copy(
            src_ref=src, dst_ref=dst, send_sem=ssem, recv_sem=rsem, device_id=dev, device_id_type=MESH
        )

    ga = g + 1 - 2 * lax.rem(g, 2)
    gb = lax.rem(g + 2, GROUP)
    gc = lax.rem(ga + 2, GROUP)
    parts = wq_parts(heads)
    part_heads = heads // parts
    part_width = width // parts

    loads = [
        pltpu.make_async_copy(src, dst, ld_s.at[n])
        for n, (src, dst) in enumerate(
            (
                (dout_h, og.at[g]),
                (source_h, source),
                (sgain_h, sgain),
                (wk_h, wk),
                (wv_h, wv),
                (target_h, target),
                (tgain_h, tgain),
                (wq_h, wq),
                (att_h, att),
            )
        )
    ]
    for load in loads:
        load.start()

    barrier = pltpu.get_barrier_semaphore()
    for o in range(1, tp_size):
        pl.semaphore_signal(barrier, inc=1, device_id=to_tp(tp_peer(o)), device_id_type=MESH)
    for o in range(1, GROUP):
        pl.semaphore_signal(barrier, inc=1, device_id=to_g(g_peer(o)), device_id_type=MESH)
    for o in range(1, outer):
        pl.semaphore_signal(barrier, inc=1, device_id=to_z(z_peer(o)), device_id_type=MESH)
    pl.semaphore_wait(barrier, tp_size + GROUP + outer - 3)

    def group_copy(k, way, slot):
        ref = (og, qg, delta)[k].at[slot]
        return copy(ref, ref, in_s.at[k, way], in_r.at[k, slot], to_g((ga, gb, ga)[way]))

    def send_own(k):
        group_copy(k, 1, g).start()
        group_copy(k, 0, g).start()

    def forward(k):
        group_copy(k, 1, gb).wait_recv()
        group_copy(k, 2, gb).start()

    def columns_copy(p, slot):
        return copy(ntt.at[:, p], nttg.at[slot], nt_s.at[p], nt_r.at[slot], to_g(p))

    loads[0].wait()
    send_own(0)
    for n in range(1, 5):
        loads[n].wait()

    s32 = source[...].astype(F32)
    ns = (s32 * inverse_rms(s32) * sgain[...]).astype(BF16)
    keys = dot_nn(ns, wk[...]).astype(BF16)
    values = dot_nn(ns, wv[...]).astype(BF16)
    for c in range(KVH):
        kvown[c, :, 0:HD] = keys[:, c * HD : (c + 1) * HD]
        kvown[c, :, HD : 2 * HD] = values[:, c * HD : (c + 1) * HD]

    def tkv(p, slot):
        return copy(kvown.at[p // per_kv], kvg.at[z, slot], tkv_s.at[p], tkv_r.at[slot], to_tp(p))

    def lkv(p, zslot, tslot):
        return copy(
            kvg.at[z, tslot], kvg.at[zslot, tslot], lkv_s.at[p, tslot], lkv_r.at[zslot, tslot], to_z(p)
        )

    for o in range(1, tp_size):
        tkv(tp_peer(o), t).start()
    kvg[z, t] = kvown[t // per_kv]
    for o in range(1, outer):
        lkv(z_peer(o), z, t).start()

    for n in range(5, 9):
        loads[n].wait()
    t32 = target[...].astype(F32)
    nt32 = t32 * inverse_rms(t32) * tgain[...]
    qg[g] = dot_nn(nt32.astype(BF16), wq[...]).astype(BF16)
    send_own(1)
    prod = (og[g].astype(F32) * att[...].astype(F32)).T
    drows = [jnp.sum(prod[h * HD : (h + 1) * HD], axis=0, keepdims=True) for h in range(heads)]
    drows.append(jnp.zeros((8 - heads, rows), F32))
    delta[g] = jnp.concatenate(drows, axis=0).astype(BF16).astype(F32)
    send_own(2)
    for o in range(1, tp_size):
        p = tp_peer(o)
        tkv(t, p).wait_recv()
        for oz in range(1, outer):
            lkv(z_peer(oz), z, p).start()
    forward(0)
    forward(1)
    forward(2)
    ntt[...] = nt32.T.astype(BF16).reshape(ntt.shape)
    for p in (gc, gb, ga):
        columns_copy(p, g).start()
    nttg[g] = ntt[:, g]
    for p in (ga, gc):
        group_copy(1, 0, p).wait_recv()

    def columns(ref, h):
        return ref[:, :, h * HD : (h + 1) * HD].reshape(group_rows, HD)

    def first(o, _):
        zc = lax.rem(z + outer - o, outer)

        @pl.when(o > 0)
        def _():
            for ts in range(tp_size):
                lkv(zc, zc, ts).wait_recv()

        kb = kvg[zc, :, :, 0:HD].reshape(block, HD)
        ktg[zc] = kb.astype(F32).T.astype(BF16)
        for h in range(heads):
            s = dot_nt(kb, columns(qg, h)) * scaling
            m = jnp.max(s, axis=0, keepdims=True)
            e = jnp.exp(s - m)
            probs[zc, h] = e
            cstat[zc, h : h + 1, :] = m
            cstat[zc, 8 + h : 9 + h, :] = jnp.sum(e, axis=0, keepdims=True)
        return 0

    lax.fori_loop(0, outer, first, 0)

    m_all = cstat[:, 0:heads, :]
    m_loc = jnp.max(m_all, axis=0)
    l_loc = jnp.sum(cstat[:, 8 : 8 + heads, :] * jnp.exp(m_all - m_loc[None]), axis=0)
    stat[g, 0:heads, :] = m_loc
    stat[g, 8 : 8 + heads, :] = l_loc
    if heads < 8:
        stat[g, heads:8, :] = jnp.zeros((8 - heads, group_rows), F32)
        stat[g, 8 + heads : 16, :] = jnp.zeros((8 - heads, group_rows), F32)

    def stat_copy(p, slot):
        return copy(stat.at[g], stat.at[slot], st_s.at[p], st_r.at[slot], to_g(p))

    for o in range(1, GROUP):
        stat_copy(g_peer(o), g).start()
    for k in (0, 2):
        for p in (ga, gc):
            group_copy(k, 0, p).wait_recv()

    def middle(zc, _):
        vb = kvg[zc, :, :, HD : 2 * HD].reshape(block, HD)
        for h in range(heads):
            drow = jnp.concatenate([delta[i, h : h + 1, :] for i in range(GROUP)], axis=1)
            prods[zc, h] = probs[zc, h] * (dot_nt(vb, columns(og, h)) - drow)
        return 0

    lax.fori_loop(0, outer, middle, 0)
    for o in range(1, GROUP):
        p = g_peer(o)
        stat_copy(p, p).wait_recv()
    m_g = jnp.max(stat[:, 0:heads, :], axis=0)
    l_g = jnp.sum(stat[:, 8 : 8 + heads, :] * jnp.exp(stat[:, 0:heads, :] - m_g[None]), axis=0)
    log_total = m_g + jnp.log(l_g)
    dqacc[...] = jnp.zeros_like(dqacc)

    def dk_copy(p, slot):
        return copy(dks.at[p], dkg.at[slot], dk_s.at[p], dk_r.at[slot], to_z(p))

    def dq_copy(k, p, slot):
        return copy(dqs.at[k, p], dqr.at[k, slot], dq_s.at[k, p], dq_r.at[k, slot], to_g(p))

    for k in range(parts):

        def second(o, _):
            zc = lax.rem(z + 1 + o, outer)
            kbt = ktg[zc]
            dk = jnp.zeros((block, HD), F32)
            dv = jnp.zeros((block, HD), F32)
            for h in range(k * part_heads, (k + 1) * part_heads):
                qh = columns(qg, h)
                oh = columns(og, h)
                factor = jnp.exp(cstat[zc, h : h + 1, :] - log_total[h : h + 1, :])
                w = probs[zc, h] * factor
                ds = (prods[zc, h] * factor).astype(BF16)
                dk = dk + dot_nn(ds, qh)
                dv = dv + dot_nn(w.astype(BF16), oh)
                dqacc[h] += dot_nn(kbt, ds)
            dk = dk * scaling
            if k > 0:
                dk = dk + dkacc[zc, :, 0:HD]
                dv = dv + dkacc[zc, :, HD : 2 * HD]
            dkacc[zc, :, 0:HD] = dk
            dkacc[zc, :, HD : 2 * HD] = dv
            if k == parts - 1:

                @pl.when(o < outer - 1)
                def _():
                    dks[zc, :, 0:HD] = dk.astype(BF16)
                    dks[zc, :, HD : 2 * HD] = dv.astype(BF16)
                    dk_copy(zc, z).start()

            return 0

        lax.fori_loop(0, outer, second, 0)

        for i in range(GROUP):
            for h in range(part_heads):
                dqs[k, i, h * HD : (h + 1) * HD] = (
                    dqacc[k * part_heads + h, :, i * rows : (i + 1) * rows] * scaling
                ).astype(BF16)
        for p in (gc, gb, ga):
            dq_copy(k, p, g).start()

    def ag_copy(k, way, slot):
        ref = dqg.at[k, slot]
        return copy(ref, ref, ag_s.at[k, way], ag_r.at[k, slot], to_g((ga, gb, ga)[way]))

    dn_term = jnp.zeros((rows, wq.shape[0]), F32)
    for k in range(parts):
        dq_sum = dqs[k, g].astype(F32)
        for p in (ga, gb, gc):
            dq_copy(k, p, p).wait_recv()
            dq_sum = dq_sum + dqr[k, p].astype(F32)
        dqg[k, g] = dq_sum.T.astype(BF16)
        ag_copy(k, 1, g).start()
        ag_copy(k, 0, g).start()

    def dn_copy(p, slot):
        return copy(dnb.at[t], dnb.at[slot], dn_s.at[p], dn_r.at[slot], to_tp(p))

    for k in range(parts):
        dn_term = dn_term + dot_nt(dqg[k, g], wq[:, k * part_width : (k + 1) * part_width])
    dnb[t] = dn_term.astype(BF16)
    for o in range(1, tp_size):
        dn_copy(tp_peer(o), t).start()
    for k in range(parts):
        ag_copy(k, 1, gb).wait_recv()
        ag_copy(k, 2, gb).start()

    def dw_copy(k, p, slot):
        return copy(dws.at[k, p], dwg.at[k, slot], dw_s.at[k, p], dw_r.at[k, slot], to_z(p))

    depth = ntt.shape[2]

    def normed_columns(i):
        return nttg[i].reshape(outer * depth, rows)

    for p in (ga, gb, gc):
        columns_copy(p, p).wait_recv()
    for k in range(parts):
        term = dot_nn(normed_columns(g), dqg[k, g]) + dot_nn(normed_columns(gb), dqg[k, gb])
        for p in (ga, gc):
            ag_copy(k, 0, p).wait_recv()
            term = term + dot_nn(normed_columns(p), dqg[k, p])
        dws[k] = term.astype(BF16).reshape(dws.shape[1:])
        for o in range(1, outer):
            dw_copy(k, z_peer(o), z).start()

    for o in range(1, outer):
        p = z_peer(o)
        dk_copy(p, p).wait_recv()
    total = dkacc[z]
    for o in range(1, outer):
        total = total + dkg[z_peer(o)].astype(F32)
    rets[...] = total.astype(BF16).reshape(rets.shape)

    def ret_copy(p, slot):
        return copy(rets.at[p], ret.at[slot], rt_s.at[p], rt_r.at[slot], to_tp(p))

    for o in range(1, tp_size):
        ret_copy(tp_peer(o), t).start()
    ret[t] = rets[t]

    stores = [
        pltpu.make_async_copy(src, dst, out_s.at[n])
        for n, (src, dst) in enumerate(((dsource, dsource_h), (dtarget, dtarget_h), (dwq, dwq_h)))
    ]
    for o in range(1, tp_size):
        p = tp_peer(o)
        dn_copy(p, p).wait_recv()
    dn = dnb[0].astype(F32)
    for k in range(1, tp_size):
        dn = dn + dnb[k].astype(F32)
    dtarget[...] = norm_back(target[...].astype(F32), tgain[...], dn).astype(BF16)

    stores[1].start()

    for o in range(1, tp_size):
        p = tp_peer(o)
        ret_copy(p, p).wait_recv()
    dns = jnp.zeros(source.shape, F32)
    for c in range(KVH):
        part = ret[c * per_kv].astype(F32)
        for k in range(1, per_kv):
            part = part + ret[c * per_kv + k].astype(F32)
        part = part.astype(BF16)
        dns = dns + dot_nt(part[:, 0:HD], wk[:, c * HD : (c + 1) * HD])
        dns = dns + dot_nt(part[:, HD : 2 * HD], wv[:, c * HD : (c + 1) * HD])
    dsource[...] = norm_back(source[...].astype(F32), sgain[...], dns)
    stores[0].start()


    for k in range(parts):
        dw_total = dws[k, z].astype(F32)
        for o in range(1, outer):
            p = z_peer(o)
            dw_copy(k, p, p).wait_recv()
            dw_total = dw_total + dwg[k, p].astype(F32)
        dwq[:, k * part_width : (k + 1) * part_width] = dw_total
    stores[2].start()

    for o in range(1, tp_size):
        p = tp_peer(o)
        tkv(p, t).wait_send()
        ret_copy(p, t).wait_send()
        dn_copy(p, t).wait_send()
    for k in range(3):
        group_copy(k, 0, g).wait_send()
        group_copy(k, 1, g).wait_send()
        group_copy(k, 2, gb).wait_send()
    for p in (ga, gb, gc):
        columns_copy(p, g).wait_send()
        stat_copy(p, g).wait_send()
        for k in range(parts):
            dq_copy(k, p, g).wait_send()
    for k in range(parts):
        ag_copy(k, 0, g).wait_send()
        ag_copy(k, 1, g).wait_send()
        ag_copy(k, 2, gb).wait_send()
    for o in range(1, outer):
        p = z_peer(o)
        for ts in range(tp_size):
            lkv(p, z, ts).wait_send()
        dk_copy(p, z).wait_send()
        for k in range(parts):
            dw_copy(k, p, z).wait_send()
    for store in stores:
        store.wait()


def wq_parts(heads):
    return 2 if heads % 2 == 0 else 1


def local(target, source, target_gain, source_gain, w_query, w_key, w_value, attended, d_attended):
    sp_size = lax.axis_size("sp")
    tp_size = lax.axis_size("tp")
    outer = sp_size // GROUP
    rows, d = target.shape
    own_rows = source.shape[0]
    block = own_rows * tp_size
    width = w_query.shape[1]
    heads = width // HD
    depth = d // sp_size
    group_rows = GROUP * rows
    vmem = pltpu.VMEM
    dma = pltpu.SemaphoreType.DMA
    parts = wq_parts(heads)
    part_width = width // parts
    scratch = [
        vmem((rows, d), BF16),
        vmem((own_rows, d), BF16),
        vmem((1, d), F32),
        vmem((1, d), F32),
        vmem((d, width), BF16),
        vmem(w_key.shape, BF16),
        vmem(w_value.shape, BF16),
        vmem((rows, width), BF16),
        vmem((rows, d), BF16),
        vmem((own_rows, d), F32),
        vmem((depth, width), F32),
        vmem((outer, HD, block), BF16),
        vmem((KVH, own_rows, 2 * HD), BF16),
        vmem((outer, tp_size, own_rows, 2 * HD), BF16),
        vmem((GROUP, rows, width), BF16),
        vmem((GROUP, rows, width), BF16),
        vmem((GROUP, 8, rows), F32),
        vmem((outer, GROUP, depth, rows), BF16),
        vmem((GROUP, outer, depth, rows), BF16),
        vmem((outer, heads, block, group_rows), F32),
        vmem((outer, heads, block, group_rows), F32),
        vmem((outer, 16, group_rows), F32),
        vmem((GROUP, 16, group_rows), F32),
        vmem((outer, block, 2 * HD), BF16),
        vmem((outer, block, 2 * HD), BF16),
        vmem((heads, HD, group_rows), F32),
        vmem((parts, GROUP, part_width, rows), BF16),
        vmem((parts, GROUP, part_width, rows), BF16),
        vmem((parts, GROUP, rows, part_width), BF16),
        vmem((tp_size, own_rows, 2 * HD), BF16),
        vmem((tp_size, own_rows, 2 * HD), BF16),
        vmem((tp_size, rows, d), BF16),
        vmem((outer, block, 2 * HD), F32),
        vmem((parts, outer, depth, part_width), BF16),
        vmem((parts, outer, depth, part_width), BF16),
    ]
    sems = [
        dma((tp_size,)),
        dma((tp_size,)),
        dma((outer, tp_size)),
        dma((outer, tp_size)),
        dma((3, 3)),
        dma((3, GROUP)),
        dma((GROUP,)),
        dma((GROUP,)),
        dma((GROUP,)),
        dma((GROUP,)),
        dma((outer,)),
        dma((outer,)),
        dma((parts, GROUP)),
        dma((parts, GROUP)),
        dma((parts, 3)),
        dma((parts, GROUP)),
        dma((tp_size,)),
        dma((tp_size,)),
        dma((tp_size,)),
        dma((tp_size,)),
        dma((parts, outer)),
        dma((parts, outer)),
        dma((9,)),
        dma((3,)),
    ]
    spec = pl.BlockSpec(memory_space=pl.ANY)
    return pl.pallas_call(
        functools.partial(kernel, sp_size, tp_size),
        out_shape=(
            jax.ShapeDtypeStruct((rows, d), BF16),
            jax.ShapeDtypeStruct((own_rows, d), F32),
            jax.ShapeDtypeStruct((depth, width), F32),
        ),
        in_specs=[spec] * 9,
        out_specs=(spec,) * 3,
        scratch_shapes=scratch + sems,
        compiler_params=pltpu.CompilerParams(
            collective_id=0, has_side_effects=True, vmem_limit_bytes=60000 * 1024
        ),
    )(
        target,
        source,
        target_gain.reshape(1, d),
        source_gain.reshape(1, d),
        w_query,
        w_key,
        w_value,
        attended,
        d_attended,
    )


def solution(mesh):
    return jax.shard_map(
        local,
        mesh=mesh,
        in_specs=(
            P("sp", None),
            P(("sp", "tp"), None),
            P(),
            P(),
            P(None, "tp"),
            P(),
            P(),
            P("sp", "tp"),
            P("sp", "tp"),
        ),
        out_specs=(P("sp", None), P(("sp", "tp"), None), P("sp", "tp")),
        check_vma=False,
    )
```
